1024 devices in a mesh: grp: 2 (over x), ep: 16 (over z), tp: 32 (over y, core).
Axes of the slice: x: 2, y: 16, z: 16, core: 2. Of those that a mesh axis runs over, the one named last changes fastest.
The devices are a block of a 4x16x16 slice.
Arguments:
- tokens: bfloat16 [2048, 2048], P(('grp', 'ep')), parts along dimension 0, may hold values from -6 to 6
- norm_gain: float32 [2048], replicated, may hold values from 0.1 to 1.9
- routes: int32 [2048, 8], P(('grp', 'ep')), parts along dimension 0, may hold values from 0 to 255, all different within a row; in each aligned block of 64 rows (0 to 63, 64 to 127, ...) at most 4 rows name the same one
- route_weight: float32 [2048, 8], P(('grp', 'ep')), parts along dimension 0, may hold values from 0.05 to 1
- gate_proj: bfloat16 [512, 2048, 256], P(('ep', 'tp')), may hold values from -0.125 to 0.125
- up_proj: bfloat16 [512, 2048, 256], P(('ep', 'tp')), may hold values from -0.125 to 0.125
- down_proj: bfloat16 [512, 256, 2048], P(('ep', 'tp')), may hold values from -0.25 to 0.25
- shared_gate: bfloat16 [2048, 512], P(None, 'tp'), may hold values from -0.125 to 0.125
- shared_up: bfloat16 [2048, 512], P(None, 'tp'), may hold values from -0.125 to 0.125
- shared_down: bfloat16 [512, 2048], P('tp'), may hold values from -0.25 to 0.25
Outputs:
- mixed: bfloat16 [2048, 2048], P(('grp', 'ep'), 'tp'), parts along dimension 0
The draws below stay inside these ranges and needn't reach their ends.
There are 2 independent parts, one for each index of `grp`. The reference program is written for one: setup_inputs(seed, part) draws one part's arguments, and reference() takes and returns one part's arrays. A program takes and returns all parts, laid end to end along the dimension named above; an argument that names none is the same for every part. Nothing has to cross between parts.
Inputs may be any that keep to these rules, and one draw needn't show every extreme that they name: `routes`: each row names 8 different experts. Among the 64 rows of one ep index no expert is named by more than 4 rows, a bound that some block reaches of them.
All inputs are finite; a program needn't handle non-finite values.
Results may differ from the reference program's by a relative error of at most 0.0064.
Values may be sent and summed in bfloat16 or wider, within the bound.
No kernel may reach another device: no remote copies, remote signals or barrier semaphores. Data moves between devices by JAX's collectives and lax.ppermute only.
A program may use at most 32 MiB of HBM per device.

```python
import math
import jax
import jax.numpy as jnp
import numpy as np
from jax import lax

D = 2048
FF = 512
SHARED = 512
TOP_K = 8
EXPERT_SHARDS = 2
TOK_DEV = 64
TOKENS = 1024
EXPERTS = 256
CAP = 4
N_EP = 16


def block_levels(key, dims, cuts, least, top_value):
    def one(dim, shards_of):
        draws = jax.random.uniform(jax.random.fold_in(jax.random.fold_in(key, 6), dim), (shards_of,), jnp.float32, least / len(cuts), top_value / len(cuts))
        return jnp.repeat(jnp.exp(draws), dims[dim] // shards_of).reshape((-1,) + (1,) * (len(dims) - dim - 1))

    factor_of = one(*cuts[0])
    for cut in cuts[1:]:
        factor_of = factor_of * one(*cut)
    return factor_of


def routed_block(rng, own, number, rows, number_of, top, limit, skew):
    order = jax.random.permutation(rng, number_of)
    heavy_load, ordinary = portions_of(number_of, rows * top, limit, skew, True), portions_of(number_of, rows * top, limit, skew, False)
    places = jnp.arange(number_of)

    def named(lengths, turn):
        used = int((lengths > 0).sum())
        fixed = max(1, used // 4)
        passed = fixed + (places - fixed + turn * (used - fixed)) % max(1, number_of - fixed)
        return jnp.zeros((number_of,), jnp.int32).at[order[jnp.where(places < fixed, places, passed)]].set(jnp.asarray(lengths, jnp.int32))

    lengths = jnp.where(number % 4 == 0, named(heavy_load, number // 4), named(ordinary, number - number // 4 - 1))
    mixed = jax.random.permutation(jax.random.fold_in(own, 3), number_of)
    giver, sink = mixed[0:number_of // 2 * 2:2], mixed[1:number_of // 2 * 2:2]
    margin = jnp.minimum(lengths[giver] - 1, limit - lengths[sink]) // 2
    margin = jnp.where((giver == order[0]) | (sink == order[0]) | (lengths[sink] == 0), 0, jnp.maximum(margin, 0))
    passed = jax.random.randint(jax.random.fold_in(own, 4), (number_of // 2,), 0, 1 << 20) % (margin + 1)
    lengths = lengths.at[giver].add(-passed).at[sink].add(passed)
    labels = jnp.searchsorted(jnp.cumsum(lengths), jnp.arange(rows * top), side="right").astype(jnp.int32)
    grid = labels.reshape(top, rows).T
    grid = grid[jax.random.permutation(jax.random.fold_in(own, 1), rows)]
    turn = jax.random.randint(jax.random.fold_in(own, 2), (rows, 1), 0, top)
    return jnp.take_along_axis(grid, (jnp.arange(top)[None, :] + turn) % top, axis=1)


def portions_of(count, total, bound, lean, full):
    weights = [(1 << 20) // math.isqrt(standing ** lean) + 1 for standing in range(1, count + 1)]
    largest = bound if full else min(bound, max(-(-total // count), total * weights[0] // sum(weights)))
    least = 1 if total - largest >= count - 1 else 0
    holding, surplus = [largest] + [least] * (count - 1), total - largest - least * (count - 1)
    while surplus > 0:
        free = [i for i in range(1, count) if holding[i] < largest] or [i for i in range(1, count) if holding[i] < bound]
        whole, remaining = sum([weights[i] for i in free]), surplus
        for i in free:
            more = min(bound - holding[i], max(1, remaining * weights[i] // whole), surplus)
            holding[i] = holding[i] + more
            surplus = surplus - more
    return np.array(holding)


def gaussian(own_key, dims, scale, most, pieces=(), dtype=jnp.bfloat16):
    level = block_levels(own_key, dims, pieces, -0.22, 0.18) if pieces else 1.0
    values = jax.random.normal(own_key, dims, jnp.float32) * scale * level
    return jnp.minimum(jnp.maximum(values, -most), most).astype(dtype)


def setup_inputs(seed: int = 0, part: int = 0) -> dict:
    streams_of = jax.random.split(jax.random.key(seed), 11)
    own_keys = jax.random.split(jax.random.fold_in(streams_of[10], part), 11)
    tokens = gaussian(own_keys[0], (TOKENS, D), 1.0, 6.0, ((0, 16),))
    norm_gain = jnp.clip(1.0 + 0.18 * jax.random.normal(streams_of[1], (D,), jnp.float32), 0.1, 1.9)
    routes_keys = jax.random.split(jax.random.fold_in(own_keys[2], 1), TOKENS // TOK_DEV)
    routes_turns = jax.random.permutation(jax.random.fold_in(own_keys[2], 3), TOKENS // TOK_DEV)
    routes = jax.vmap(lambda own, number: routed_block(jax.random.fold_in(own_keys[2], 2), own, number, TOK_DEV, EXPERTS, TOP_K, CAP, 2))(routes_keys, routes_turns).reshape((TOKENS, TOP_K))
    route_weight = jnp.clip(jnp.exp(math.log(1.0) - 2.9957323 * jax.random.uniform(own_keys[3], (TOKENS, TOP_K), jnp.float32) ** block_levels(own_keys[3], (TOKENS, TOP_K), ((0, 16),), -0.2, 0.2)), 0.05, 1.0)
    gate_proj = gaussian(streams_of[4], (EXPERTS * EXPERT_SHARDS, D, FF // EXPERT_SHARDS), D ** -0.5, 0.125, ((0, 512),))
    up_proj = gaussian(streams_of[5], (EXPERTS * EXPERT_SHARDS, D, FF // EXPERT_SHARDS), D ** -0.5, 0.125, ((0, 512),))
    down_proj = gaussian(streams_of[6], (EXPERTS * EXPERT_SHARDS, FF // EXPERT_SHARDS, D), FF ** -0.5, 0.25, ((0, 512),))
    shared_gate = gaussian(streams_of[7], (D, SHARED), D ** -0.5, 0.125, ((1, 32),))
    shared_up = gaussian(streams_of[8], (D, SHARED), D ** -0.5, 0.125, ((1, 32),))
    shared_down = gaussian(streams_of[9], (SHARED, D), SHARED ** -0.5, 0.25, ((0, 32),))
    return {"tokens": tokens, "norm_gain": norm_gain, "routes": routes, "route_weight": route_weight, "gate_proj": gate_proj, "up_proj": up_proj, "down_proj": down_proj, "shared_gate": shared_gate, "shared_up": shared_up, "shared_down": shared_down}


eps = 1e-06
routed_scale = 2.5

def expert_apply(row_block, gate_half, up_half, down_half):
    gate_part = jnp.dot(row_block, gate_half, preferred_element_type=jnp.float32)
    upper = jnp.dot(row_block, up_half, preferred_element_type=jnp.float32)
    active = (jax.nn.silu(gate_part) * upper).astype(jnp.bfloat16)
    return jnp.dot(active, down_half, preferred_element_type=jnp.float32)

def reference(tokens, norm_gain, routes, route_weight, gate_proj, up_proj, down_proj, shared_gate, shared_up, shared_down):
    values = tokens.astype(jnp.float32)
    scaled = values * lax.rsqrt(lax.optimization_barrier(jnp.mean(values * values, axis=-1, keepdims=True)) + eps)
    normed = (scaled * norm_gain).astype(jnp.bfloat16)
    mixing = route_weight / lax.optimization_barrier(jnp.sum(route_weight, axis=1, keepdims=True)) * routed_scale
    row_limit = N_EP * CAP

    def one_expert(expert_id, total):
        expert_id = jnp.asarray(expert_id).astype(jnp.int32)
        hit_table = routes == expert_id
        taken_rows = jnp.any(hit_table, axis=1)
        token_weight = lax.optimization_barrier(jnp.sum(jnp.where(hit_table, mixing, 0.0), axis=1))
        picked = jnp.nonzero(taken_rows, size=row_limit, fill_value=0)[0].astype(jnp.int32)
        live_rows = jnp.arange(row_limit) < jnp.sum(taken_rows.astype(jnp.int32))
        row_block = normed[picked]
        produced = jnp.zeros((row_limit, D), jnp.float32)
        for half_index in range(EXPERT_SHARDS):
            weight_row = (expert_id * EXPERT_SHARDS + half_index).astype(jnp.int32)
            gate_half = lax.dynamic_index_in_dim(gate_proj, weight_row, 0, keepdims=False)
            up_half = lax.dynamic_index_in_dim(up_proj, weight_row, 0, keepdims=False)
            down_half = lax.dynamic_index_in_dim(down_proj, weight_row, 0, keepdims=False)
            produced = produced + expert_apply(row_block, gate_half, up_half, down_half)
        scale_rows = jnp.where(live_rows, token_weight[picked], 0.0)
        return total.at[picked].add(produced * scale_rows[:, None])
    routed = lax.fori_loop(0, EXPERTS, one_expert, jnp.zeros((TOKENS, D), jnp.float32))
    shared_term = expert_apply(normed, shared_gate, shared_up, shared_down)
    return (routed + shared_term).astype(jnp.bfloat16)
```

```python
import functools

import jax
import jax.numpy as jnp
from jax import lax
from jax.experimental import pallas as pl
from jax.experimental.pallas import tpu as pltpu
from jax.sharding import PartitionSpec as P

EXPERT_SHARDS = 2
LANES = 128
HALF = LANES // 2

eps = 1e-06
routed_scale = 2.5

VMEM = pl.BlockSpec(memory_space=pltpu.VMEM)
SMEM = pl.BlockSpec(memory_space=pltpu.SMEM)


def call(kernel, outs, in_specs, name, flops, mib=16):
    return pl.pallas_call(
        kernel,
        out_shape=outs,
        in_specs=in_specs,
        out_specs=jax.tree.map(lambda _: VMEM, outs),
        compiler_params=pltpu.CompilerParams(vmem_limit_bytes=mib << 20),
        cost_estimate=pl.CostEstimate(flops=flops, bytes_accessed=1 << 20, transcendentals=0),
        name=name,
    )


def hits_of(routes_t, targets):
    hit = routes_t[0:1, :] == targets
    for j in range(1, routes_t.shape[0]):
        hit = hit | (routes_t[j : j + 1, :] == targets)
    return hit


def slots_of(hit):
    tokens = hit.shape[1]
    before = lax.broadcasted_iota(jnp.int32, (tokens, tokens), 0)
    after = lax.broadcasted_iota(jnp.int32, (tokens, tokens), 1)
    lower = jnp.where(before <= after, 1.0, 0.0).astype(jnp.bfloat16)
    ones = jnp.where(hit, 1.0, 0.0).astype(jnp.bfloat16)
    return jnp.dot(ones, lower, preferred_element_type=jnp.float32)


def row_parts(rows, tokens, capacity):
    row = lax.broadcasted_iota(jnp.int32, (rows, tokens), 0)
    peer = row // (2 * capacity)
    half = (row // capacity) % 2
    slot = row % capacity
    return peer, half, slot


def select_rows(col_ref, routes_t, rows, tokens, capacity, per_block):
    peer, half, slot = row_parts(rows, tokens, capacity)
    hit = hits_of(routes_t, peer * per_block + col_ref[0])
    counts = slots_of(hit)
    return hit & (counts == (slot + 1).astype(jnp.float32)), half


def dispatch_kernel(capacity, per_block, col_ref, routes_ref, tokens_ref, gain_ref, out_ref, normed_ref):
    values = tokens_ref[...].astype(jnp.float32)
    width = values.shape[1]
    scale = lax.rsqrt(jnp.sum(values * values, axis=-1, keepdims=True) * (1.0 / width) + eps)
    normed = (values * scale * gain_ref[...]).astype(jnp.bfloat16)
    normed_ref[...] = normed
    tokens = values.shape[0]
    rows = out_ref.shape[0]
    chosen, half = select_rows(col_ref, routes_ref[...], rows, tokens, capacity, per_block)
    first = jnp.where(chosen & (half == 0), 1.0, 0.0).astype(jnp.bfloat16)
    second = jnp.where(chosen & (half == 1), 1.0, 0.0).astype(jnp.bfloat16)
    low, high = normed[:, : width // 2], normed[:, width // 2 :]
    out = jnp.dot(first, low, preferred_element_type=jnp.float32)
    out = out + jnp.dot(second, high, preferred_element_type=jnp.float32)
    out_ref[...] = out.astype(jnp.bfloat16)


def silu_times(gate, up):
    return (gate / (1.0 + jnp.exp(-gate)) * up).astype(jnp.bfloat16)


def split_by_core(core, full):
    rows, width = full.shape
    lane = lax.broadcasted_iota(jnp.int32, (rows, LANES), 1)
    low = lane < HALF
    mine, theirs = [], []
    for j in range(0, width // LANES, 2):
        even = full[:, j * LANES : (j + 1) * LANES]
        odd = full[:, (j + 1) * LANES : (j + 2) * LANES]
        firsts = jnp.where(low, even, pltpu.roll(odd, HALF, 1))
        lasts = jnp.where(low, pltpu.roll(even, HALF, 1), odd)
        mine.append(jnp.where(core == 0, firsts, lasts))
        theirs.append(jnp.where(core == 0, lasts, firsts))
    return jnp.concatenate(mine, axis=1), jnp.concatenate(theirs, axis=1)


def side_kernel(
    capacity, per_block, col_ref, routes_ref, weight_ref, normed_ref, gate_ref, up_ref, down_ref,
    weights_ref, mine_ref, theirs_ref,
):
    routes_t = routes_ref[...]
    weight_t = weight_ref[...]
    mixing = weight_t / jnp.sum(weight_t, axis=0, keepdims=True) * routed_scale
    choices, tokens = routes_t.shape
    rows = weights_ref.shape[1]
    chosen, half = select_rows(col_ref, routes_t, rows, tokens, capacity, per_block)
    peer, _, _ = row_parts(rows, tokens, capacity)
    target = peer * per_block + col_ref[0]
    scale = jnp.zeros((rows, tokens), jnp.float32)
    for j in range(choices):
        scale = scale + jnp.where(routes_t[j : j + 1, :] == target, mixing[j : j + 1, :], 0.0)
    for h in range(2):
        table = jnp.where(chosen & (half == h), scale, 0.0)
        top = table.astype(jnp.bfloat16)
        rest = (table - top.astype(jnp.float32)).astype(jnp.bfloat16)
        weights_ref[h] = jnp.concatenate([top, rest], axis=1)
    normed = normed_ref[...]
    contract = (((1,), (1,)), ((), ()))
    gate = lax.dot_general(normed, gate_ref[...], contract, preferred_element_type=jnp.float32)
    up = lax.dot_general(normed, up_ref[...], contract, preferred_element_type=jnp.float32)
    active = silu_times(gate, up)
    full = jnp.dot(active, down_ref[...], preferred_element_type=jnp.float32)
    mine, theirs = split_by_core(col_ref[1], full)
    mine_ref[...] = mine
    theirs_ref[...] = theirs.astype(jnp.bfloat16)


def expert_kernel(
    capacity, col_ref, rows_ref, gate_ref, up_ref, down_ref, shared_ref, mine_ref, theirs_ref
):
    x = rows_ref[...]
    rows, depth = x.shape

    def product(weights):
        low = jnp.dot(x, weights[:depth], preferred_element_type=jnp.float32)
        high = jnp.dot(x, weights[depth:], preferred_element_type=jnp.float32)
        return low + pltpu.roll(high, rows - capacity, 0)

    active = silu_times(product(gate_ref[0]), product(up_ref[0]))
    full = jnp.dot(active, down_ref[0], preferred_element_type=jnp.float32)
    mine, theirs = split_by_core(col_ref[1], full)
    half = mine.shape[1] // 2
    row = lax.broadcasted_iota(jnp.int32, (rows, half), 0)
    first = (row // capacity) % 2 == 0

    def fold(v):
        return jnp.where(first, v[:, :half], pltpu.roll(v[:, half:], capacity, 0))

    mine_ref[...] = fold(mine)
    theirs_ref[:rows] = fold(theirs).astype(jnp.bfloat16)
    shared = shared_ref[...]
    tokens = shared.shape[0]
    theirs_ref[rows : rows + tokens] = shared[:, :half]
    theirs_ref[rows + tokens :] = shared[:, half:]


def pair_kernel(mine_ref, theirs_ref, out_ref):
    rows = mine_ref.shape[0]
    out_ref[...] = (mine_ref[...] + theirs_ref[:rows].astype(jnp.float32)).astype(jnp.bfloat16)


def combine_kernel(returned_ref, weights_ref, shared_ref, theirs_ref, out_ref):
    returned = returned_ref[...]
    rows, half = returned.shape
    tokens = shared_ref.shape[0]
    contract = (((0,), (0,)), ((), ()))
    halves = []
    for h in range(2):
        both = lax.dot_general(weights_ref[h], returned, contract, preferred_element_type=jnp.float32)
        routed = both[:tokens] + both[tokens:]
        first = rows + h * tokens
        shared = shared_ref[:, h * half : (h + 1) * half] + theirs_ref[first : first + tokens].astype(jnp.float32)
        halves.append(routed + shared)
    total = jnp.concatenate(halves, axis=1)
    part = tokens // 2
    low = lax.broadcasted_iota(jnp.int32, (part, LANES), 1) < HALF
    for j in range(total.shape[1] // LANES):
        tile = total[:, j * LANES : (j + 1) * LANES]
        turned = pltpu.roll(tile, HALF, 1)
        even = jnp.where(low, tile[:part], turned[part:])
        odd = jnp.where(low, turned[:part], tile[part:])
        out_ref[2 * j * part : (2 * j + 1) * part] = even.astype(jnp.bfloat16)
        out_ref[(2 * j + 1) * part : (2 * j + 2) * part] = odd.astype(jnp.bfloat16)


def final_kernel(count, parts_ref, out_ref):
    part = parts_ref.shape[0] // count
    total = parts_ref[:part].astype(jnp.float32)
    for i in range(1, count):
        total = total + parts_ref[i * part : (i + 1) * part].astype(jnp.float32)
    turned = pltpu.roll(total, HALF, 1)
    out_ref[:part] = total[:, :HALF].astype(jnp.bfloat16)
    out_ref[part:] = turned[:, :HALF].astype(jnp.bfloat16)


def per_device(
    tokens,
    norm_gain,
    routes,
    route_weight,
    gate_proj,
    up_proj,
    down_proj,
    shared_gate,
    shared_up,
    shared_down,
):
    ep_count = lax.axis_size("ep")
    tp_count = lax.axis_size("tp")
    per_block = tp_count // EXPERT_SHARDS
    experts = ep_count * per_block
    tok_rows, top_count = routes.shape
    width = tokens.shape[1]
    capacity = min(tok_rows, max(2, 2 * tok_rows * top_count // experts))
    rows = ep_count * 2 * capacity
    tp = lax.axis_index("tp")
    place = jnp.stack([tp // EXPERT_SHARDS, tp % EXPERT_SHARDS]).astype(jnp.int32)
    routes_t, weight_t = routes.T, route_weight.T
    f32, bf16 = jnp.float32, jnp.bfloat16
    shape = jax.ShapeDtypeStruct

    with jax.named_scope("dispatch"):
        outgoing, normed = call(
            functools.partial(dispatch_kernel, capacity, per_block),
            (shape((rows, width // 2), bf16), shape((tok_rows, width), bf16)),
            [SMEM, VMEM, VMEM, VMEM],
            "dispatch",
            1 << 27,
        )(place, routes_t, tokens, norm_gain.reshape(1, width))
        arrived = lax.all_to_all(
            outgoing.reshape(ep_count, 2 * capacity, width // 2), "ep", 0, 0, tiled=True
        )
    with jax.named_scope("side"):
        weights, shared_mine, shared_theirs = call(
            functools.partial(side_kernel, capacity, per_block),
            (
                shape((2, rows, 2 * tok_rows), bf16),
                shape((tok_rows, width // 2), f32),
                shape((tok_rows, width // 2), bf16),
            ),
            [SMEM] + [VMEM] * 6,
            "side",
            1 << 30,
        )(place, routes_t, weight_t, normed, shared_gate.T, shared_up.T, shared_down)
    with jax.named_scope("experts"):
        mine, theirs = call(
            functools.partial(expert_kernel, capacity),
            (shape((rows, width // 4), f32), shape((rows + 2 * tok_rows, width // 4), bf16)),
            [SMEM] + [VMEM] * 5,
            "experts",
            1 << 28,
        )(place, arrived.reshape(rows, width // 2), gate_proj, up_proj, down_proj, shared_theirs)
    with jax.named_scope("pair"):
        theirs = lax.ppermute(theirs, "tp", [(i, i ^ 1) for i in range(tp_count)])
        produced = call(pair_kernel, shape((rows, width // 4), bf16), [VMEM] * 2, "pair", 1 << 20)(mine, theirs)
    with jax.named_scope("back"):
        returned = lax.all_to_all(
            produced.reshape(ep_count, 2 * capacity, width // 4), "ep", 0, 0, tiled=True
        )
    with jax.named_scope("combine"):
        sums = call(
            combine_kernel,
            shape((per_block * tok_rows // 2, LANES), bf16),
            [VMEM] * 4,
            "combine",
            1 << 26,
        )(returned.reshape(rows, width // 4), weights, shared_mine, theirs)
        groups = [list(range(core, tp_count, EXPERT_SHARDS)) for core in range(EXPERT_SHARDS)]
        parts = lax.all_to_all(
            sums.reshape(per_block, tok_rows // 2, LANES), "tp", 0, 0, tiled=True, axis_index_groups=groups
        )
    with jax.named_scope("final"):
        return call(
            functools.partial(final_kernel, per_block),
            shape((tok_rows, width // tp_count), bf16),
            [VMEM],
            "final",
            1 << 20,
        )(parts.reshape(per_block * tok_rows // 2, LANES))


def solution(mesh):
    in_specs = (
        P(("grp", "ep"), None),
        P(),
        P(("grp", "ep"), None),
        P(("grp", "ep"), None),
        P(("ep", "tp"), None, None),
        P(("ep", "tp"), None, None),
        P(("ep", "tp"), None, None),
        P(None, "tp"),
        P(None, "tp"),
        P("tp", None),
    )
    out_specs = P(("grp", "ep"), "tp")
    return jax.shard_map(
        per_device, mesh=mesh, in_specs=in_specs, out_specs=out_specs, check_vma=False
    )
```

```python
import functools

import jax
import jax.numpy as jnp
from jax import lax
from jax.experimental import pallas as pl
from jax.experimental.pallas import tpu as pltpu
from jax.sharding import PartitionSpec as P


EXPERT_SHARDS = 2
LANES = 128
HALF = LANES // 2

eps = 1e-06
routed_scale = 2.5

VMEM = pl.BlockSpec(memory_space=pltpu.VMEM)
HBM = pl.BlockSpec(memory_space=pltpu.HBM)


def call(kernel, outs, in_specs, flops, mib=16, scratch=()):
    return pl.pallas_call(
        kernel,
        out_shape=outs,
        in_specs=in_specs,
        out_specs=jax.tree.map(lambda _: VMEM, outs),
        scratch_shapes=scratch,
        compiler_params=pltpu.CompilerParams(vmem_limit_bytes=mib << 20),
        cost_estimate=pl.CostEstimate(flops=flops, bytes_accessed=1 << 20, transcendentals=0),
    )


QUARTERS = 4


def hits_of(routes_t, targets):
    hit = routes_t[0:1, :] == targets
    for j in range(1, routes_t.shape[0]):
        hit = hit | (routes_t[j : j + 1, :] == targets)
    return hit


def slots_of(hit):
    tokens = hit.shape[1]
    before = lax.broadcasted_iota(jnp.int32, (tokens, tokens), 0)
    after = lax.broadcasted_iota(jnp.int32, (tokens, tokens), 1)
    lower = jnp.where(before <= after, 1.0, 0.0).astype(jnp.bfloat16)
    ones = jnp.where(hit, 1.0, 0.0).astype(jnp.bfloat16)
    return jnp.dot(ones, lower, preferred_element_type=jnp.float32)


def iota(rows, columns, dim):
    return lax.broadcasted_iota(jnp.int32, (rows, columns), dim)


def one_hot(mask):
    return jnp.where(mask, 1.0, 0.0).astype(jnp.bfloat16)


def stack_quarters(full):
    part = full.shape[1] // QUARTERS
    return jnp.concatenate([full[:, q * part : (q + 1) * part] for q in range(QUARTERS)], axis=0)


def spread_quarters(stacked):
    part = stacked.shape[0] // QUARTERS
    return jnp.concatenate([stacked[q * part : (q + 1) * part] for q in range(QUARTERS)], axis=1)


def stay(value):
    return pltpu.with_memory_space_constraint(value, pltpu.HBM)


def own_place():
    tp = lax.axis_index("tp")
    return tp // EXPERT_SHARDS, tp % EXPERT_SHARDS


def norm_rows(tokens, gain):
    values = tokens.astype(jnp.float32)
    scale = lax.rsqrt(jnp.sum(values * values, axis=-1, keepdims=True) * (1.0 / values.shape[1]) + eps)
    return (values * scale * gain).astype(jnp.bfloat16)


def fetch(pairs, sems):
    copies = [pltpu.make_async_copy(a, b, sems.at[i]) for i, (a, b) in enumerate(pairs)]
    for copy in copies:
        copy.start()
    return copies


def dispatch_kernel(
    slots, per_block, routes_hbm, tokens_hbm, gain_hbm, out_ref, routes_ref, tokens_ref, gain_ref, sems
):
    copies = fetch(((routes_hbm, routes_ref), (gain_hbm, gain_ref), (tokens_hbm, tokens_ref)), sems)
    column, core = own_place()
    copies[0].wait()
    tokens = tokens_ref.shape[0]
    rows = out_ref.shape[0]
    row = iota(rows, tokens, 0)
    peer, quarter = row // (QUARTERS * slots), (row // slots) % QUARTERS
    slot = core * slots + row % slots
    hit = hits_of(routes_ref[...], peer * per_block + column)
    chosen = hit & (slots_of(hit) == (slot + 1).astype(jnp.float32))
    table = jnp.concatenate([one_hot(chosen & (quarter == q)) for q in range(QUARTERS)], axis=1)
    copies[1].wait()
    copies[2].wait()
    normed = norm_rows(tokens_ref[...], gain_ref[...])
    out = jnp.dot(table, stack_quarters(normed), preferred_element_type=jnp.float32)
    out_ref[...] = out.astype(jnp.bfloat16)


def silu_times(gate, up):
    return (gate / (1.0 + jnp.exp(-gate)) * up).astype(jnp.bfloat16)


def split_by_core(full):
    rows, width = full.shape
    low = iota(rows, LANES, 1) < HALF
    firsts, lasts = [], []
    for j in range(0, width // LANES, 2):
        even = full[:, j * LANES : (j + 1) * LANES]
        odd = full[:, (j + 1) * LANES : (j + 2) * LANES]
        firsts.append(jnp.where(low, even, pltpu.roll(odd, HALF, 1)))
        lasts.append(jnp.where(low, pltpu.roll(even, HALF, 1), odd))
    return jnp.concatenate(firsts, axis=1), jnp.concatenate(lasts, axis=1)


def side_kernel(
    slots, per_block, routes_hbm, weight_hbm, tokens_hbm, gain_hbm, gate_hbm, up_hbm, down_hbm,
    table_ref, shared_ref, routes_ref, weight_ref, tokens_ref, gain_ref, gate_ref, up_ref, down_ref, sems,
):
    copies = fetch(
        (
            (routes_hbm, routes_ref), (weight_hbm, weight_ref), (tokens_hbm, tokens_ref), (gain_hbm, gain_ref),
            (gate_hbm, gate_ref), (up_hbm, up_ref), (down_hbm, down_ref),
        ),
        sems,
    )
    column, core = own_place()
    for copy in copies:
        copy.wait()
    routes_t = routes_ref[...]
    weight_t = weight_ref[...]
    mixing = weight_t / jnp.sum(weight_t, axis=0, keepdims=True) * routed_scale
    choices, tokens = routes_t.shape
    rows = table_ref.shape[1]
    row = iota(rows, tokens, 0)
    target = row // (QUARTERS * slots) * per_block + column
    slot = core * slots + row % slots
    hit = hits_of(routes_t, target)
    chosen = hit & (slots_of(hit) == (slot + 1).astype(jnp.float32))
    scale = jnp.zeros((rows, tokens), jnp.float32)
    for j in range(choices):
        scale = scale + jnp.where(routes_t[j : j + 1, :] == target, mixing[j : j + 1, :], 0.0)
    table = jnp.where(chosen, scale, 0.0).T
    quarter = (iota(tokens, rows, 1) // slots) % QUARTERS
    for q in range(QUARTERS):
        part = jnp.where(quarter == q, table, 0.0)
        top = part.astype(jnp.bfloat16)
        table_ref[q * tokens : (q + 1) * tokens] = top
        rest = (part - top.astype(jnp.float32)).astype(jnp.bfloat16)
        table_ref[(QUARTERS + q) * tokens : (QUARTERS + q + 1) * tokens] = rest
    normed = norm_rows(tokens_ref[...], gain_ref[...])
    contract = (((1,), (1,)), ((), ()))
    gate = lax.dot_general(normed, gate_ref[...], contract, preferred_element_type=jnp.float32)
    up = lax.dot_general(normed, up_ref[...], contract, preferred_element_type=jnp.float32)
    shared_ref[...] = jnp.dot(silu_times(gate, up), down_ref[...], preferred_element_type=jnp.float32)


def expert_kernel(
    slots, rows_ref, gate_ref, up_ref, gate_two_ref, up_two_hbm, down_hbm, down_two_hbm, out_ref,
    up_two_ref, down_ref, down_two_ref, sems,
):
    copies = fetch(((up_two_hbm, up_two_ref), (down_hbm, down_ref), (down_two_hbm, down_two_ref)), sems)
    arrived = rows_ref[...]
    total = arrived.shape[0]
    kept = total // QUARTERS
    to, source = iota(total, total, 0), iota(total, total, 1)
    place = to % kept // slots * (QUARTERS * slots) + to // kept * slots + to % slots
    sorted_rows = jnp.dot(one_hot(source == place), arrived, preferred_element_type=jnp.float32)
    x = spread_quarters(sorted_rows.astype(jnp.bfloat16))

    def product(weights):
        return jnp.dot(x, weights[0], preferred_element_type=jnp.float32)

    active = silu_times(product(gate_ref), product(up_ref))
    gate_two = product(gate_two_ref)
    copies[0].wait()
    active_two = silu_times(gate_two, product(up_two_ref))
    copies[1].wait()
    full = jnp.dot(active, down_ref[0], preferred_element_type=jnp.float32)
    copies[2].wait()
    full = full + jnp.dot(active_two, down_two_ref[0], preferred_element_type=jnp.float32)
    pieces = stack_quarters(full).astype(jnp.bfloat16)
    to, source = iota(total, total, 0), iota(total, total, 1)
    place = to // slots % QUARTERS * kept + to // (QUARTERS * slots) * slots + to % slots
    out = jnp.dot(one_hot(source == place), pieces, preferred_element_type=jnp.float32)
    out_ref[...] = out.astype(jnp.bfloat16)


def combine_kernel(returned_ref, table_ref, shared_ref, mine_ref, theirs_ref):
    both = jnp.dot(table_ref[...], returned_ref[...], preferred_element_type=jnp.float32)
    part = both.shape[0] // 2
    total = spread_quarters(both[:part] + both[part:]) + shared_ref[...]
    firsts, lasts = split_by_core(total)
    _, core = own_place()
    mine_ref[...] = jnp.where(core == 0, firsts, lasts)
    theirs_ref[...] = jnp.where(core == 0, lasts, firsts).astype(jnp.bfloat16)


def pair_kernel(mine_ref, theirs_ref, out_ref):
    total = mine_ref[...] + theirs_ref[...].astype(jnp.float32)
    part = total.shape[0] // 2
    low = iota(part, LANES, 1) < HALF
    for j in range(total.shape[1] // LANES):
        tile = total[:, j * LANES : (j + 1) * LANES]
        turned = pltpu.roll(tile, HALF, 1)
        even = jnp.where(low, tile[:part], turned[part:])
        odd = jnp.where(low, turned[:part], tile[part:])
        out_ref[2 * j * part : (2 * j + 1) * part] = even.astype(jnp.bfloat16)
        out_ref[(2 * j + 1) * part : (2 * j + 2) * part] = odd.astype(jnp.bfloat16)


def final_kernel(count, parts_ref, out_ref):
    part = parts_ref.shape[0] // count
    total = parts_ref[:part].astype(jnp.float32)
    for i in range(1, count):
        total = total + parts_ref[i * part : (i + 1) * part].astype(jnp.float32)
    turned = pltpu.roll(total, HALF, 1)
    out_ref[:part] = total[:, :HALF].astype(jnp.bfloat16)
    out_ref[part:] = turned[:, :HALF].astype(jnp.bfloat16)


def per_device(
    tokens,
    norm_gain,
    routes,
    route_weight,
    gate_proj,
    up_proj,
    down_proj,
    shared_gate,
    shared_up,
    shared_down,
):
    ep_count = lax.axis_size("ep")
    tp_count = lax.axis_size("tp")
    per_block = tp_count // EXPERT_SHARDS
    experts = ep_count * per_block
    tok_rows, top_count = routes.shape
    width = tokens.shape[1]
    capacity = min(tok_rows, max(2, 2 * tok_rows * top_count // experts))
    slots = capacity // EXPERT_SHARDS
    routes_t, weight_t = routes.T, route_weight.T
    gain = norm_gain.reshape(1, width)
    f32, bf16 = jnp.float32, jnp.bfloat16
    shape = jax.ShapeDtypeStruct
    partners = [(i, i ^ 1) for i in range(tp_count)]

    chunk = slots * QUARTERS
    rows = ep_count * chunk
    outgoing = call(
        functools.partial(dispatch_kernel, slots, per_block),
        shape((rows, width // QUARTERS), bf16),
        [HBM] * 3,
        1 << 27,
        scratch=[
            pltpu.VMEM(routes_t.shape, routes.dtype),
            pltpu.VMEM(tokens.shape, tokens.dtype),
            pltpu.VMEM(gain.shape, gain.dtype),
            pltpu.SemaphoreType.DMA((3,)),
        ],
    )(stay(routes_t), stay(tokens), stay(gain))
    arrived = lax.all_to_all(
        outgoing.reshape(ep_count, chunk, width // QUARTERS), "ep", 0, 0, tiled=True
    )
    operands = (routes_t, weight_t, tokens, gain, shared_gate.T, shared_up.T, shared_down)
    table, shared = call(
        functools.partial(side_kernel, slots, per_block),
        (
            shape((2 * QUARTERS * tok_rows, rows), bf16),
            shape((tok_rows, width), f32),
        ),
        [HBM] * len(operands),
        1 << 29,
        scratch=[pltpu.VMEM(v.shape, v.dtype) for v in operands]
        + [pltpu.SemaphoreType.DMA((len(operands),))],
    )(*map(stay, operands))
    gate_two = lax.ppermute(gate_proj, "tp", partners)
    up_two = lax.ppermute(up_proj, "tp", partners)
    down_two = lax.ppermute(down_proj, "tp", partners)
    part = width // QUARTERS
    produced = call(
        functools.partial(expert_kernel, slots),
        shape((rows, part), bf16),
        [VMEM] * 4 + [HBM] * 3,
        1 << 28,
        scratch=[pltpu.VMEM(v.shape, v.dtype) for v in (up_proj, down_proj, down_proj)]
        + [pltpu.SemaphoreType.DMA((3,))],
    )(
        arrived.reshape(rows, part), gate_proj, up_proj, gate_two,
        stay(up_two), stay(down_proj), stay(down_two),
    )
    returned = lax.all_to_all(produced.reshape(ep_count, chunk, part), "ep", 0, 0, tiled=True)
    mine, theirs = call(
        combine_kernel, (shape((tok_rows, width // 2), f32), shape((tok_rows, width // 2), bf16)), [VMEM] * 3, 1 << 26
    )(returned.reshape(rows, part), table, shared)
    theirs = lax.ppermute(theirs, "tp", partners)
    sums = call(pair_kernel, shape((per_block * tok_rows // 2, LANES), bf16), [VMEM] * 2, 1 << 20)(mine, theirs)
    groups = [list(range(core, tp_count, EXPERT_SHARDS)) for core in range(EXPERT_SHARDS)]
    parts = lax.all_to_all(
        sums.reshape(per_block, tok_rows // 2, LANES), "tp", 0, 0, tiled=True, axis_index_groups=groups
    )
    return call(
        functools.partial(final_kernel, per_block), shape((tok_rows, width // tp_count), bf16), [VMEM], 1 << 20
    )(parts.reshape(per_block * tok_rows // 2, LANES))


def solution(mesh):
    in_specs = (
        P(("grp", "ep"), None),
        P(),
        P(("grp", "ep"), None),
        P(("grp", "ep"), None),
        P(("ep", "tp"), None, None),
        P(("ep", "tp"), None, None),
        P(("ep", "tp"), None, None),
        P(None, "tp"),
        P(None, "tp"),
        P("tp", None),
    )
    out_specs = P(("grp", "ep"), "tp")
    return jax.shard_map(
        per_device, mesh=mesh, in_specs=in_specs, out_specs=out_specs, check_vma=False
    )
```
